32 devices in a mesh: grp: 2 (over y), sp: 4 (over z), tp: 4 (over x, core).
Axes of the slice: x: 2, y: 2, z: 4, core: 2. Of those that a mesh axis runs over, the one named last changes fastest.
Arguments:
- queries: bfloat16 [6144, 1024], P(('grp', 'sp'), 'tp'), parts along dimension 0, may hold values from -160 to 160
- key_rows: bfloat16 [6144, 256], P(('grp', 'sp'), 'tp'), parts along dimension 0, may hold values from -4 to 4
- value_rows: bfloat16 [6144, 256], P(('grp', 'sp'), 'tp'), parts along dimension 0, may hold values from -5 to 5
- sink_logits: float32 [16], P('tp'), may hold values from 2 to 6
- out_weight: bfloat16 [1024, 2048], replicated, may hold values from -0.75 to 0.75
- residual: bfloat16 [6144, 2048], P(('grp', 'sp', 'tp')), parts along dimension 0, may hold values from -6 to 6
- norm_gain: float32 [2048], replicated, may hold values from 0.1 to 1.9
- up_weight: bfloat16 [2048, 4096], P('sp', 'tp'), may hold values from -0.125 to 0.125
- down_weight: bfloat16 [4096, 2048], P('tp', 'sp'), may hold values from -0.09375 to 0.09375
Outputs:
- layer_out: bfloat16 [6144, 2048], P(('grp', 'sp', 'tp')), parts along dimension 0
The draws below stay inside these ranges and needn't reach their ends.
There are 2 independent parts, one for each index of `grp`. The reference program is written for one: setup_inputs(seed, part) draws one part's arguments, and reference() takes and returns one part's arrays. A program takes and returns all parts, laid end to end along the dimension named above; an argument that names none is the same for every part. Nothing has to cross between parts.
All inputs are finite; a program needn't handle non-finite values.
Results may differ from the reference program's by a relative error of at most 0.017.
Values may be sent and summed in bfloat16 or wider, within the bound.
A program may use at most 64 MiB of HBM per device.

```python
import jax
import jax.numpy as jnp
from jax import lax

D = 2048
Q_HEADS = 16
KV_HEADS = 4
HEAD_DIM = 64
FF = 4096
WINDOW = 128
TOKENS = 3072
N_TP = 4


def attention_base(key):
    query_key = jax.random.fold_in(key, 11)
    row_key = jax.random.fold_in(key, 12)
    keys_raw = jax.random.truncated_normal(row_key, -4.0, 4.0, (TOKENS, KV_HEADS, HEAD_DIM), jnp.float32)
    queries_raw = jax.random.truncated_normal(query_key, -4.0, 4.0, (TOKENS, Q_HEADS, HEAD_DIM), jnp.float32)
    return (queries_raw, keys_raw)


def draw_queries(key, part):
    return attention_base(key)[0].reshape(TOKENS, Q_HEADS * HEAD_DIM).astype(jnp.bfloat16)


def draw_key_rows(key, part):
    return attention_base(key)[1].reshape(TOKENS, KV_HEADS * HEAD_DIM).astype(jnp.bfloat16)


def shard_levels(own_key, dims, cuts, least, largest):
    gain = 1.0
    for axis_at, blocks in cuts:
        heights = jax.random.uniform(jax.random.fold_in(jax.random.fold_in(own_key, 6), axis_at), (blocks,), jnp.float32, least / len(cuts), largest / len(cuts))
        gain = gain * jnp.repeat(jnp.exp(heights), dims[axis_at] // blocks).reshape((-1,) + (1,) * (len(dims) - 1 - axis_at))
    return gain


def scatter_about(own_key, dims, scale, bound, shards=(), kind=jnp.bfloat16):
    entries = jax.random.normal(own_key, dims, jnp.float32) * scale
    if len(shards) > 0:
        entries = shard_levels(own_key, dims, shards, -0.22, 0.18) * entries
    return jnp.clip(entries, min=-bound, max=bound).astype(kind)


def setup_inputs(seed: int = 0, part: int = 0) -> dict:
    streams_of = jax.random.split(jax.random.key(seed), 10)
    own_keys = jax.random.split(jax.random.fold_in(streams_of[9], part), 10)
    queries = draw_queries(jax.random.fold_in(jax.random.fold_in(streams_of[9], part), 71), part)
    key_rows = draw_key_rows(jax.random.fold_in(jax.random.fold_in(streams_of[9], part), 71), part)
    value_rows = scatter_about(own_keys[2], (TOKENS, KV_HEADS * HEAD_DIM), 1.0, 5.0, ((0, 4), (1, 4)))
    sink_logits = jnp.clip(2.0 + 4.0 * jax.random.uniform(streams_of[3], (Q_HEADS,), jnp.float32) ** shard_levels(streams_of[3], (Q_HEADS,), ((0, 4),), -0.2, 0.2), 2.0, 6.0)
    out_weight = scatter_about(streams_of[4], (Q_HEADS * HEAD_DIM, D), (Q_HEADS * HEAD_DIM // 16) ** -0.5, 0.75)
    residual = scatter_about(own_keys[5], (TOKENS, D), 1.0, 6.0, ((0, 16),))
    norm_gain = jnp.clip(1.0 + 0.18 * jax.random.normal(streams_of[6], (D,), jnp.float32), 0.1, 1.9)
    up_weight = scatter_about(streams_of[7], (D, FF), D ** -0.5, 0.125, ((0, 4), (1, 4)))
    down_weight = scatter_about(streams_of[8], (FF, D), FF ** -0.5, 0.09375, ((0, 4), (1, 4)))
    return {"queries": queries, "key_rows": key_rows, "value_rows": value_rows, "sink_logits": sink_logits, "out_weight": out_weight, "residual": residual, "norm_gain": norm_gain, "up_weight": up_weight, "down_weight": down_weight}


def band_attend(queries, key_rows, value_rows, sink_logits):
    rows = queries.shape[0]
    group = queries.shape[1] // HEAD_DIM
    blocks = rows // WINDOW
    zero_tail = jnp.zeros((WINDOW, HEAD_DIM), jnp.float32)
    all_keys = jnp.concatenate([zero_tail, key_rows.astype(jnp.float32)], axis=0).reshape(blocks + 1, WINDOW, HEAD_DIM)
    all_values = jnp.concatenate([zero_tail, value_rows.astype(jnp.float32)], axis=0).reshape(blocks + 1, WINDOW, HEAD_DIM)
    key_blocks = jnp.concatenate([all_keys[:-1], all_keys[1:]], axis=1)
    value_blocks = jnp.concatenate([all_values[:-1], all_values[1:]], axis=1)
    query_blocks = queries.astype(jnp.float32).reshape(blocks, WINDOW, group, HEAD_DIM)
    scores = jnp.einsum('nqgd,nsd->ngqs', query_blocks, key_blocks) * HEAD_DIM ** (-0.5)
    q_local = jnp.arange(WINDOW, dtype=jnp.int32) + WINDOW
    k_local = jnp.arange(2 * WINDOW, dtype=jnp.int32)
    distance = q_local[:, None] - k_local[None, :]
    key_position = (jnp.arange(blocks, dtype=jnp.int32)[:, None] - 1) * WINDOW + k_local[None, :]
    valid = ((distance >= 0) & (distance < WINDOW))[None] & (key_position >= 0)[:, None, :]
    scores = jnp.where(valid[:, None], scores, -1e+30)
    sink = sink_logits.astype(jnp.float32)[None, :, None, None]
    top = jnp.maximum(lax.optimization_barrier(jnp.max(scores, axis=-1, keepdims=True)), sink)
    weights = jnp.exp(scores - top)
    total = lax.optimization_barrier(jnp.sum(weights, axis=-1, keepdims=True)) + jnp.exp(sink - top)
    probs = (weights / total).astype(jnp.bfloat16).astype(jnp.float32)
    result = jnp.einsum('ngqs,nsd->nqgd', probs, value_blocks)
    return result.astype(jnp.bfloat16).reshape(rows, group * HEAD_DIM)

def reference(queries, key_rows, value_rows, sink_logits, out_weight, residual, norm_gain, up_weight, down_weight):
    group = Q_HEADS // KV_HEADS
    pieces = []
    for head in range(KV_HEADS):
        pieces.append(band_attend(queries[:, head * group * HEAD_DIM:(head + 1) * group * HEAD_DIM], key_rows[:, head * HEAD_DIM:(head + 1) * HEAD_DIM], value_rows[:, head * HEAD_DIM:(head + 1) * HEAD_DIM], sink_logits[head * group:(head + 1) * group]))
    attended = jnp.concatenate(pieces, axis=1)
    projected = jnp.dot(attended, out_weight, preferred_element_type=jnp.float32)
    mixed = (residual.astype(jnp.float32) + projected).astype(jnp.bfloat16)
    mixed32 = mixed.astype(jnp.float32)
    scale = lax.rsqrt(lax.optimization_barrier(jnp.mean(mixed32 * mixed32, axis=-1, keepdims=True)) + 1e-06)
    normed = (mixed32 * scale * norm_gain).astype(jnp.bfloat16)
    hidden = jnp.square(jax.nn.relu(jnp.dot(normed, up_weight, preferred_element_type=jnp.float32))).astype(jnp.bfloat16)
    width = FF // N_TP
    down = jnp.zeros((TOKENS, D), jnp.float32)
    for index in range(N_TP):
        partial_product = jnp.dot(hidden[:, index * width:(index + 1) * width], down_weight[index * width:(index + 1) * width], preferred_element_type=jnp.float32).astype(jnp.bfloat16)
        down = down + lax.optimization_barrier(partial_product).astype(jnp.float32)
    return (mixed32 + down).astype(jnp.bfloat16)
```

```python
import functools

import jax
import jax.numpy as jnp
from jax import lax
from jax.experimental import pallas as pl
from jax.experimental.pallas import tpu as pltpu
from jax.sharding import PartitionSpec as P

HEAD_DIM = 64
WINDOW = 128


def shifted(value, axis, steps):
    count = lax.axis_size(axis)
    leading, last = (max(0, -steps), min(count, count - steps))
    return lax.ppermute(value, axis, [(source, source + steps) for source in range(leading, last)])


def band_attend(queries, key_rows, value_rows, sink_logits, tail_keys, tail_values, offset):
    rows = queries.shape[0]
    kv_heads = key_rows.shape[1] // HEAD_DIM
    group = queries.shape[1] // (kv_heads * HEAD_DIM)
    blocks = rows // WINDOW
    all_keys = jnp.concatenate([tail_keys, key_rows], axis=0).reshape(
        blocks + 1, WINDOW, kv_heads, HEAD_DIM
    )
    all_values = jnp.concatenate([tail_values, value_rows], axis=0).reshape(
        blocks + 1, WINDOW, kv_heads, HEAD_DIM
    )
    key_blocks = jnp.concatenate([all_keys[:-1], all_keys[1:]], axis=1)
    value_blocks = jnp.concatenate([all_values[:-1], all_values[1:]], axis=1)
    query_blocks = queries.reshape(blocks, WINDOW, kv_heads, group, HEAD_DIM)
    scores = jnp.einsum(
        "nqkgd,nskd->nkgqs", query_blocks, key_blocks, preferred_element_type=jnp.float32
    ) * HEAD_DIM ** (-0.5)
    q_local = jnp.arange(WINDOW, dtype=jnp.int32) + WINDOW
    k_local = jnp.arange(2 * WINDOW, dtype=jnp.int32)
    distance = q_local[:, None] - k_local[None, :]
    key_position = (
        offset + (jnp.arange(blocks, dtype=jnp.int32)[:, None] - 1) * WINDOW + k_local[None, :]
    )
    valid = ((distance >= 0) & (distance < WINDOW))[None] & (key_position >= 0)[:, None, :]
    scores = jnp.where(valid[:, None, None], scores, -1e30)
    sink = sink_logits.reshape(kv_heads, group)[None, :, :, None, None]
    top = jnp.maximum(jnp.max(scores, axis=-1, keepdims=True), sink)
    weights = jnp.exp(scores - top)
    total = jnp.sum(weights, axis=-1, keepdims=True) + jnp.exp(sink - top)
    probs = (weights / total).astype(jnp.bfloat16)
    result = jnp.einsum(
        "nkgqs,nskd->nqkgd", probs, value_blocks, preferred_element_type=jnp.float32
    )
    return result.astype(jnp.bfloat16).reshape(rows, kv_heads * group * HEAD_DIM)


def body(
    queries,
    key_rows,
    value_rows,
    sink_logits,
    out_weight,
    residual,
    norm_gain,
    up_weight,
    down_weight,
):
    rows = queries.shape[0]
    width = key_rows.shape[1]
    kv_pair = jnp.concatenate([key_rows[rows - WINDOW :], value_rows[rows - WINDOW :]], axis=1)
    tail = shifted(kv_pair, "sp", 1)
    offset = lax.axis_index("sp") * rows
    attended = band_attend(
        queries, key_rows, value_rows, sink_logits, tail[:, :width], tail[:, width:], offset
    )
    head_cols = attended.shape[1]
    own_rows = lax.dynamic_slice_in_dim(out_weight, lax.axis_index("tp") * head_cols, head_cols, 0)
    projected = lax.psum_scatter(
        jnp.dot(attended, own_rows, preferred_element_type=jnp.float32).astype(jnp.bfloat16),
        "tp",
        scatter_dimension=0,
        tiled=True,
    ).astype(jnp.float32)
    mixed32 = (residual.astype(jnp.float32) + projected).astype(jnp.bfloat16).astype(jnp.float32)
    scale = lax.rsqrt(jnp.mean(mixed32 * mixed32, axis=-1, keepdims=True) + 1e-06)
    normed = (mixed32 * scale * norm_gain).astype(jnp.bfloat16)
    all_rows = lax.all_gather(normed, "tp", axis=0, tiled=True)
    before = jnp.dot(
        all_rows,
        lax.all_gather(up_weight, "sp", axis=0, tiled=True),
        preferred_element_type=jnp.float32,
    )
    hidden = jnp.square(jax.nn.relu(before)).astype(jnp.bfloat16)
    terms = jnp.dot(
        hidden,
        lax.all_gather(down_weight, "sp", axis=1, tiled=True),
        preferred_element_type=jnp.float32,
    )
    down = lax.psum_scatter(
        terms.astype(jnp.bfloat16), "tp", scatter_dimension=0, tiled=True
    ).astype(jnp.float32)
    return (mixed32 + down).astype(jnp.bfloat16)


CHUNKS = 4
F32 = jnp.float32
BF16 = jnp.bfloat16


def remote(src, dst, send_sem, recv_sem, device_id):
    return pltpu.make_async_remote_copy(
        src_ref=src,
        dst_ref=dst,
        send_sem=send_sem,
        recv_sem=recv_sem,
        device_id=device_id,
        device_id_type=pl.DeviceIdType.MESH,
    )


def aligned(value, size):
    return pl.multiple_of(value * size, size)


def layer_kernel(
    n,
    queries,
    keys,
    values,
    sink,
    out_weight,
    residual,
    gain,
    up,
    down,
    out,
    q_buf,
    k_buf,
    v_buf,
    k_wide,
    v_wide,
    attended,
    att_all,
    ow_buf,
    res_buf,
    mixed,
    normed,
    up_buf,
    down_buf,
    acc,
    hidden,
    terms,
    pair_in,
    chip_sum,
    peer_in,
    local_sem,
    tail_send,
    tail_recv,
    z_send,
    y_send,
    w_recv,
    att_send,
    att_recv,
    norm_send,
    norm_recv,
    pair_send,
    pair_recv,
    peer_send,
    peer_recv,
):
    z = lax.axis_index("sp")
    y = lax.axis_index("grp")
    me = lax.axis_index("tp")
    partner = me + 1 - 2 * lax.rem(me, 2)
    across = lax.rem(me + 2, 4)
    diagonal = lax.rem(partner + 2, 4)
    rows, head_cols = q_buf.shape
    own = rows // 4
    depth = up.shape[0]
    width = down.shape[1]
    cols = up.shape[1]
    wide = n * width
    chunk = (depth // 2 // CHUNKS, down.shape[0] // 2 // CHUNKS)

    barrier = pltpu.get_barrier_semaphore()
    for step in range(1, 4):
        pl.semaphore_signal(
            barrier,
            inc=1,
            device_id={"tp": lax.rem(me + step, 4)},
            device_id_type=pl.DeviceIdType.MESH,
        )
    pl.semaphore_signal(
        barrier, inc=1, device_id={"grp": 1 - y}, device_id_type=pl.DeviceIdType.MESH
    )

    @pl.when(z > 0)
    def _():
        pl.semaphore_signal(
            barrier, inc=1, device_id={"sp": z - 1}, device_id_type=pl.DeviceIdType.MESH
        )

    @pl.when(z < n - 1)
    def _():
        pl.semaphore_signal(
            barrier, inc=1, device_id={"sp": z + 1}, device_id_type=pl.DeviceIdType.MESH
        )

    own_up = up_buf.at[pl.ds(aligned(z, depth), depth), :]
    locals_ = [
        pltpu.make_async_copy(keys, k_buf.at[pl.ds(WINDOW, rows), :], local_sem.at[0]),
        pltpu.make_async_copy(values, v_buf.at[pl.ds(WINDOW, rows), :], local_sem.at[1]),
        pltpu.make_async_copy(queries, q_buf, local_sem.at[2]),
        pltpu.make_async_copy(out_weight, ow_buf, local_sem.at[3]),
        pltpu.make_async_copy(residual, res_buf, local_sem.at[4]),
        pltpu.make_async_copy(up, own_up, local_sem.at[5]),
        pltpu.make_async_copy(down, down_buf.at[z], local_sem.at[6]),
    ]
    for copy in locals_:
        copy.start()

    edge = jnp.where(z > 0, 1, 0) + jnp.where(z < n - 1, 1, 0)
    pl.semaphore_wait(barrier, 4 + edge)

    def piece(weight, owner, half, index):
        if weight == 0:
            start = owner * depth + half * (depth // 2) + index * chunk[0]
            return up_buf.at[pl.ds(pl.multiple_of(start, chunk[0]), chunk[0]), :]
        start = half * (CHUNKS * chunk[1]) + index * chunk[1]
        return down_buf.at[owner, pl.ds(pl.multiple_of(start, chunk[1]), chunk[1]), :]

    def own_piece(weight, index):
        start = y * (CHUNKS * chunk[weight]) + index * chunk[weight]
        ref = up if weight == 0 else down
        return ref.at[pl.ds(pl.multiple_of(start, chunk[weight]), chunk[weight]), :]

    def z_copy(weight, owner, index, upward, source=None):
        place = piece(weight, owner, y, index)
        return remote(
            place if source is None else source,
            place,
            z_send.at[upward, weight, owner, index],
            w_recv.at[weight, owner, y, index],
            {"sp": z + (1 if upward else -1)},
        )

    def y_copy(weight, owner, index):
        place = piece(weight, owner, y, index)
        return remote(
            place,
            place,
            y_send.at[weight, owner, index],
            w_recv.at[weight, owner, y, index],
            {"grp": 1 - y},
        )

    def wait_piece(weight, owner, half, index):
        place = piece(weight, owner, half, index)
        remote(
            place,
            place,
            y_send.at[weight, owner, index],
            w_recv.at[weight, owner, half, index],
            {"grp": 1 - y},
        ).wait_recv()

    def send_own(weight, upward):
        for index in range(CHUNKS):
            z_copy(weight, z, index, upward, own_piece(weight, index)).start()

    def tail_copy(which):
        source, place = ((keys, k_buf), (values, v_buf))[which]
        return remote(
            source.at[pl.ds(rows - WINDOW, WINDOW), :],
            place.at[pl.ds(0, WINDOW), :],
            tail_send.at[which],
            tail_recv.at[which],
            {"sp": z + 1},
        )

    @pl.when(z < n - 1)
    def _():
        tail_copy(0).start()
        tail_copy(1).start()
        send_own(0, 1)

    @pl.when(z > 0)
    def _():
        send_own(0, 0)

    def send_down(stage):
        @pl.when((z == stage) & (z < n - 1))
        def _():
            send_own(1, 1)

        @pl.when((n - 1 - z == stage) & (z > 0))
        def _():
            send_own(1, 0)

    send_down(0)

    near = jnp.minimum(z, n - 1 - z)
    far_sign = jnp.where(z < n - 1 - z, 1, -1)

    def owner_at(order):
        close = order <= 2 * near
        side = 2 * lax.rem(order + 1, 2) - 1
        return z + jnp.where(close, side * ((order + 1) // 2), far_sign * (order - near))

    def event(weight, number):
        span = 2 * CHUNKS
        close = number < near * span
        rest = number - near * span
        side = 2 * (number % 2) - 1
        owner = z + jnp.where(
            close,
            side * (number // span + 1),
            far_sign * (near + 1 + lax.div(jnp.maximum(rest, 0), CHUNKS)),
        )
        index = jnp.where(
            close, (number % span) // 2, lax.rem(jnp.maximum(rest, 0), CHUNKS)
        )
        wait_piece(weight, owner, y, index)

        @pl.when((owner < z) & (z < n - 1))
        def _():
            z_copy(weight, owner, index, 1).start()

        @pl.when((owner > z) & (z > 0))
        def _():
            z_copy(weight, owner, index, 0).start()

        y_copy(weight, owner, index).start()

    total_events = (n - 1) * CHUNKS
    done = [0, 0]

    def pump(weight, until):
        while done[weight] < min(until, total_events):
            event(weight, done[weight])
            done[weight] += 1
            if weight == 0:
                for stage in range(1, n - 1):
                    if done[0] == min(stage * 2 * CHUNKS, total_events):
                        send_down(stage)

    @pl.when(z == 0)
    def _():
        k_buf[pl.ds(0, WINDOW), :] = jnp.zeros((WINDOW, HEAD_DIM), BF16)
        v_buf[pl.ds(0, WINDOW), :] = jnp.zeros((WINDOW, HEAD_DIM), BF16)

    for copy in locals_[:3]:
        copy.wait()

    @pl.when(z > 0)
    def _():
        tail_copy(0).wait_recv()
        tail_copy(1).wait_recv()

    heads = head_cols // HEAD_DIM
    spread = jnp.where(
        lax.broadcasted_iota(jnp.int32, (HEAD_DIM, head_cols), 1) % HEAD_DIM
        == lax.broadcasted_iota(jnp.int32, (HEAD_DIM, head_cols), 0),
        1.0,
        0.0,
    ).astype(BF16)
    k_wide[...] = jnp.dot(k_buf[...], spread, preferred_element_type=F32).astype(BF16)
    v_wide[...] = jnp.dot(v_buf[...], spread, preferred_element_type=F32).astype(BF16)

    def attend(block, carry):
        start = aligned(block, WINDOW)
        q_rows = q_buf[pl.ds(start, WINDOW), :].astype(F32)
        lane_head = lax.broadcasted_iota(jnp.int32, (WINDOW, head_cols), 1) // HEAD_DIM
        stacked = jnp.concatenate(
            [jnp.where(lane_head == h, q_rows, 0.0) for h in range(heads)], axis=0
        ).astype(BF16)
        scores = lax.dot_general(
            stacked,
            k_wide[pl.ds(start, 2 * WINDOW), :],
            (((1,), (1,)), ((), ())),
            preferred_element_type=F32,
        ) * HEAD_DIM ** (-0.5)
        i = lax.broadcasted_iota(jnp.int32, (heads * WINDOW, 2 * WINDOW), 0) % WINDOW
        j = lax.broadcasted_iota(jnp.int32, (heads * WINDOW, 2 * WINDOW), 1)
        first = WINDOW - z * rows - block * WINDOW
        valid = (j > i) & (j <= i + WINDOW) & (j >= first)
        scores = jnp.where(valid, scores, -1e30)
        sinks = jnp.concatenate(
            [jnp.full((WINDOW, 1), sink[h], F32) for h in range(heads)], axis=0
        )
        top = jnp.maximum(jnp.max(scores, axis=-1, keepdims=True), sinks)
        weights = jnp.exp(scores - top)
        total = jnp.sum(weights, axis=-1, keepdims=True) + jnp.exp(sinks - top)
        probs = (weights / total).astype(BF16)
        mixed_heads = jnp.dot(
            probs, v_wide[pl.ds(start, 2 * WINDOW), :], preferred_element_type=F32
        )
        result = jnp.zeros((WINDOW, head_cols), F32)
        for h in range(heads):
            result += jnp.where(
                lane_head == h, mixed_heads[h * WINDOW : (h + 1) * WINDOW], 0.0
            )
        attended[pl.ds(start, WINDOW), :] = result.astype(BF16)
        return carry

    blocks = rows // WINDOW
    for block in range(0, blocks, 2):
        lax.fori_loop(block, min(block + 2, blocks), attend, 0)
        pump(0, block // 2 + 1)

    def att_copy(step):
        peer = lax.rem(me + step, 4)
        return remote(
            attended.at[pl.ds(aligned(peer, own), own), :],
            att_all.at[me],
            att_send.at[step - 1],
            att_recv.at[me],
            {"tp": peer},
        )

    def att_wait(step):
        peer = lax.rem(me + step, 4)
        remote(
            att_all.at[peer], att_all.at[peer], att_send.at[step - 1], att_recv.at[peer], {"tp": peer}
        ).wait_recv()

    for step in (2, 1, 3):
        att_copy(step).start()
    att_all[me] = attended[pl.ds(aligned(me, own), own), :]
    pump(0, 4)
    locals_[3].wait()
    locals_[4].wait()
    for step in (1, 2, 3):
        att_wait(step)

    tile = 256

    def project(index, squares):
        span = pl.ds(aligned(index, tile), tile)
        value = res_buf[:, span].astype(F32)
        for peer in range(4):
            value += jnp.dot(
                att_all[peer],
                ow_buf[peer * head_cols : (peer + 1) * head_cols, span],
                preferred_element_type=F32,
            )
        value = value.astype(BF16).astype(F32)
        mixed[:, span] = value
        return squares + jnp.sum(value * value, axis=-1, keepdims=True)

    squares = lax.fori_loop(0, wide // tile, project, jnp.zeros((own, 1), F32))
    scale = lax.rsqrt(squares / wide + 1e-06)
    own_rows = pl.ds(aligned(me, own), own)

    def normalize(index, carry):
        span = pl.ds(aligned(index, tile), tile)
        normed[own_rows, span] = (mixed[:, span] * scale * gain[:, span]).astype(BF16)
        return carry

    lax.fori_loop(0, wide // tile, normalize, 0)

    def norm_copy(slot, source, target):
        place = normed.at[pl.ds(aligned(source, own), own), :]
        return remote(place, place, norm_send.at[slot], norm_recv.at[source], {"tp": target})

    norm_copy(0, me, across).start()
    norm_copy(1, me, partner).start()
    pump(0, 3 * total_events // 4)
    norm_copy(2, across, across).wait_recv()
    norm_copy(2, across, partner).start()
    pump(0, total_events)

    locals_[5].wait()
    norm_copy(2, partner, partner).wait_recv()
    norm_copy(2, diagonal, partner).wait_recv()

    for order in range(n):
        owner = owner_at(order) if order else z
        if order:
            for index in range(CHUNKS):
                wait_piece(0, owner, 1 - y, index)

        def up_step(index, carry, owner=owner, order=order):
            span = pl.ds(aligned(index, tile), tile)
            value = jnp.dot(
                normed[:, pl.ds(aligned(owner, depth), depth)],
                up_buf[pl.ds(aligned(owner, depth), depth), span],
                preferred_element_type=F32,
            )
            if order:
                value += acc[:, span]
            if order == n - 1:
                hidden[:, span] = jnp.square(jnp.maximum(value, 0.0)).astype(BF16)
            else:
                acc[:, span] = value
            return carry

        lax.fori_loop(0, cols // tile, up_step, 0)
        if order == n - 2:
            pump(1, CHUNKS)

    def pair_copy(order, slot):
        group = (partner, diagonal)[slot]
        return remote(
            terms.at[order, pl.ds(aligned(group, own), own), :],
            pair_in.at[order, slot],
            pair_send.at[order, slot],
            pair_recv.at[order, slot],
            {"tp": partner},
        )

    def peer_copy(order):
        return remote(
            chip_sum.at[order],
            peer_in.at[order],
            peer_send.at[order],
            peer_recv.at[order],
            {"tp": across},
        )

    def finish(order):
        owner = owner_at(order) if order else z
        span = pl.ds(aligned(owner, width), width)
        peer_copy(order).wait_recv()
        pair_copy(order, 0).wait_recv()
        total = (
            terms[order, own_rows, :].astype(F32)
            + pair_in[order, 0].astype(F32)
            + peer_in[order].astype(F32)
        )
        out[:, span] = (mixed[:, span] + total).astype(BF16)

    locals_[6].wait()
    for order in range(n):
        owner = owner_at(order) if order else z
        if order:
            pump(1, (order + 1) * CHUNKS if order % 2 else order * CHUNKS)
            for index in range(CHUNKS):
                wait_piece(1, owner, 1 - y, index)

        def down_step(index, carry, owner=owner, order=order):
            span = pl.ds(aligned(index, tile), tile)
            terms[order, :, span] = jnp.dot(
                hidden[...], down_buf[owner, :, span], preferred_element_type=F32
            ).astype(BF16)
            return carry

        lax.fori_loop(0, width // tile, down_step, 0)
        pair_copy(order, 1).start()
        pair_copy(order, 0).start()
        pair_copy(order, 1).wait_recv()
        other = pl.ds(aligned(across, own), own)
        chip_sum[order] = (
            terms[order, other, :].astype(F32) + pair_in[order, 1].astype(F32)
        ).astype(BF16)
        peer_copy(order).start()
        if order:
            finish(order - 1)
    finish(n - 1)

    for step in (1, 2, 3):
        att_copy(step).wait_send()
    norm_copy(0, me, across).wait_send()
    norm_copy(1, me, partner).wait_send()
    norm_copy(2, across, partner).wait_send()
    for order in range(n):
        pair_copy(order, 0).wait_send()
        pair_copy(order, 1).wait_send()
        peer_copy(order).wait_send()

    @pl.when(z < n - 1)
    def _():
        tail_copy(0).wait_send()
        tail_copy(1).wait_send()

    for weight in range(2):
        for owner in range(n):

            @pl.when((z >= owner) & (z < n - 1))
            def _():
                for index in range(CHUNKS):
                    z_copy(weight, owner, index, 1).wait_send()

            @pl.when((z <= owner) & (z > 0))
            def _():
                for index in range(CHUNKS):
                    z_copy(weight, owner, index, 0).wait_send()

            @pl.when(z != owner)
            def _():
                for index in range(CHUNKS):
                    y_copy(weight, owner, index).wait_send()


def fused_body(
    n,
    queries,
    key_rows,
    value_rows,
    sink_logits,
    out_weight,
    residual,
    norm_gain,
    up_weight,
    down_weight,
):
    rows, head_cols = queries.shape
    own, wide = residual.shape
    depth, cols = up_weight.shape
    width = down_weight.shape[1]
    vmem = lambda *shape: pltpu.VMEM(shape, BF16)
    dma = lambda *shape: pltpu.SemaphoreType.DMA(shape)
    hbm = pl.BlockSpec(memory_space=pl.ANY)
    return pl.pallas_call(
        functools.partial(layer_kernel, n),
        out_shape=jax.ShapeDtypeStruct((own, wide), BF16),
        in_specs=[
            hbm,
            hbm,
            hbm,
            pl.BlockSpec(memory_space=pltpu.SMEM),
            hbm,
            hbm,
            pl.BlockSpec(memory_space=pltpu.VMEM),
            hbm,
            hbm,
        ],
        out_specs=pl.BlockSpec(memory_space=pltpu.VMEM),
        scratch_shapes=[
            vmem(rows, head_cols),
            vmem(rows + WINDOW, HEAD_DIM),
            vmem(rows + WINDOW, HEAD_DIM),
            vmem(rows + WINDOW, head_cols),
            vmem(rows + WINDOW, head_cols),
            vmem(rows, head_cols),
            vmem(4, own, head_cols),
            vmem(*out_weight.shape),
            vmem(own, wide),
            pltpu.VMEM((own, wide), F32),
            vmem(rows, wide),
            vmem(n * depth, cols),
            vmem(n, cols, width),
            pltpu.VMEM((rows, cols), F32),
            vmem(rows, cols),
            vmem(n, rows, width),
            vmem(n, 2, own, width),
            vmem(n, own, width),
            vmem(n, own, width),
            dma(7),
            dma(2),
            dma(2),
            dma(2, 2, n, CHUNKS),
            dma(2, n, CHUNKS),
            dma(2, n, 2, CHUNKS),
            dma(3),
            dma(4),
            dma(3),
            dma(4),
            dma(n, 2),
            dma(n, 2),
            dma(n),
            dma(n),
        ],
        compiler_params=pltpu.CompilerParams(
            collective_id=0, has_side_effects=True, vmem_limit_bytes=60 * 1024 * 1024
        ),
    )(
        queries,
        key_rows,
        value_rows,
        sink_logits,
        out_weight,
        residual,
        norm_gain.reshape(1, -1),
        up_weight,
        down_weight,
    )


def solution(mesh):
    in_specs = (
        P(("grp", "sp"), "tp"),
        P(("grp", "sp"), "tp"),
        P(("grp", "sp"), "tp"),
        P("tp"),
        P(),
        P(("grp", "sp", "tp"), None),
        P(),
        P("sp", "tp"),
        P("tp", "sp"),
    )
    out_specs = P(("grp", "sp", "tp"), None)
    n = mesh.shape["sp"]
    shards_fit = 2 <= n <= 8

    def layer(*arrays):
        key_rows, up_weight, down_weight = arrays[1], arrays[7], arrays[8]
        fits = (
            shards_fit
            and mesh.shape["grp"] == 2
            and mesh.shape["tp"] == 4
            and key_rows.shape[1] == HEAD_DIM
            and up_weight.shape[0] % (32 * CHUNKS) == 0
            and up_weight.shape[1] % 256 == 0
            and down_weight.shape[1] % 256 == 0
        )
        return (functools.partial(fused_body, n) if fits else body)(*arrays)

    return jax.shard_map(layer, mesh=mesh, in_specs=in_specs, out_specs=out_specs, check_vma=False)
```

```python
import functools

import jax
import jax.numpy as jnp
from jax import lax
from jax.experimental import pallas as pl
from jax.experimental.pallas import tpu as pltpu
from jax.sharding import PartitionSpec as P

HEAD_DIM = 64
WINDOW = 128


def shifted(value, axis, steps):
    count = lax.axis_size(axis)
    leading, last = (max(0, -steps), min(count, count - steps))
    return lax.ppermute(value, axis, [(source, source + steps) for source in range(leading, last)])


def band_attend(queries, key_rows, value_rows, sink_logits, tail_keys, tail_values, offset):
    rows = queries.shape[0]
    kv_heads = key_rows.shape[1] // HEAD_DIM
    group = queries.shape[1] // (kv_heads * HEAD_DIM)
    blocks = rows // WINDOW
    all_keys = jnp.concatenate([tail_keys, key_rows], axis=0).reshape(
        blocks + 1, WINDOW, kv_heads, HEAD_DIM
    )
    all_values = jnp.concatenate([tail_values, value_rows], axis=0).reshape(
        blocks + 1, WINDOW, kv_heads, HEAD_DIM
    )
    key_blocks = jnp.concatenate([all_keys[:-1], all_keys[1:]], axis=1)
    value_blocks = jnp.concatenate([all_values[:-1], all_values[1:]], axis=1)
    query_blocks = queries.reshape(blocks, WINDOW, kv_heads, group, HEAD_DIM)
    scores = jnp.einsum(
        "nqkgd,nskd->nkgqs", query_blocks, key_blocks, preferred_element_type=jnp.float32
    ) * HEAD_DIM ** (-0.5)
    q_local = jnp.arange(WINDOW, dtype=jnp.int32) + WINDOW
    k_local = jnp.arange(2 * WINDOW, dtype=jnp.int32)
    distance = q_local[:, None] - k_local[None, :]
    key_position = (
        offset + (jnp.arange(blocks, dtype=jnp.int32)[:, None] - 1) * WINDOW + k_local[None, :]
    )
    valid = ((distance >= 0) & (distance < WINDOW))[None] & (key_position >= 0)[:, None, :]
    scores = jnp.where(valid[:, None, None], scores, -1e30)
    sink = sink_logits.reshape(kv_heads, group)[None, :, :, None, None]
    top = jnp.maximum(jnp.max(scores, axis=-1, keepdims=True), sink)
    weights = jnp.exp(scores - top)
    total = jnp.sum(weights, axis=-1, keepdims=True) + jnp.exp(sink - top)
    probs = (weights / total).astype(jnp.bfloat16)
    result = jnp.einsum(
        "nkgqs,nskd->nqkgd", probs, value_blocks, preferred_element_type=jnp.float32
    )
    return result.astype(jnp.bfloat16).reshape(rows, kv_heads * group * HEAD_DIM)


def body(
    queries,
    key_rows,
    value_rows,
    sink_logits,
    out_weight,
    residual,
    norm_gain,
    up_weight,
    down_weight,
):
    rows = queries.shape[0]
    width = key_rows.shape[1]
    kv_pair = jnp.concatenate([key_rows[rows - WINDOW :], value_rows[rows - WINDOW :]], axis=1)
    tail = shifted(kv_pair, "sp", 1)
    offset = lax.axis_index("sp") * rows
    attended = band_attend(
        queries, key_rows, value_rows, sink_logits, tail[:, :width], tail[:, width:], offset
    )
    head_cols = attended.shape[1]
    own_rows = lax.dynamic_slice_in_dim(out_weight, lax.axis_index("tp") * head_cols, head_cols, 0)
    projected = lax.psum_scatter(
        jnp.dot(attended, own_rows, preferred_element_type=jnp.float32).astype(jnp.bfloat16),
        "tp",
        scatter_dimension=0,
        tiled=True,
    ).astype(jnp.float32)
    mixed32 = (residual.astype(jnp.float32) + projected).astype(jnp.bfloat16).astype(jnp.float32)
    scale = lax.rsqrt(jnp.mean(mixed32 * mixed32, axis=-1, keepdims=True) + 1e-06)
    normed = (mixed32 * scale * norm_gain).astype(jnp.bfloat16)
    all_rows = lax.all_gather(normed, "tp", axis=0, tiled=True)
    before = jnp.dot(
        all_rows,
        lax.all_gather(up_weight, "sp", axis=0, tiled=True),
        preferred_element_type=jnp.float32,
    )
    hidden = jnp.square(jax.nn.relu(before)).astype(jnp.bfloat16)
    terms = jnp.dot(
        hidden,
        lax.all_gather(down_weight, "sp", axis=1, tiled=True),
        preferred_element_type=jnp.float32,
    )
    down = lax.psum_scatter(
        terms.astype(jnp.bfloat16), "tp", scatter_dimension=0, tiled=True
    ).astype(jnp.float32)
    return (mixed32 + down).astype(jnp.bfloat16)


CHUNKS = 4
LEAD = 2
F32 = jnp.float32
BF16 = jnp.bfloat16


def remote(src, dst, send_sem, recv_sem, device_id):
    return pltpu.make_async_remote_copy(
        src_ref=src,
        dst_ref=dst,
        send_sem=send_sem,
        recv_sem=recv_sem,
        device_id=device_id,
        device_id_type=pl.DeviceIdType.MESH,
    )


def aligned(value, size):
    return pl.multiple_of(value * size, size)


def layer_kernel(
    n,
    queries,
    keys,
    values,
    sink,
    out_weight,
    residual,
    gain,
    up,
    down,
    out,
    q_buf,
    k_buf,
    v_buf,
    k_wide,
    v_wide,
    attended,
    att_all,
    ow_buf,
    res_buf,
    mixed,
    normed,
    up_buf,
    down_buf,
    acc,
    hidden,
    terms,
    pair_in,
    chip_sum,
    peer_in,
    local_sem,
    tail_send,
    tail_recv,
    z_send,
    y_send,
    w_recv,
    att_send,
    att_recv,
    norm_send,
    norm_recv,
    pair_send,
    pair_recv,
    peer_send,
    peer_recv,
):
    z = lax.axis_index("sp")
    y = lax.axis_index("grp")
    me = lax.axis_index("tp")
    partner = me + 1 - 2 * lax.rem(me, 2)
    across = lax.rem(me + 2, 4)
    diagonal = lax.rem(partner + 2, 4)
    rows, head_cols = q_buf.shape
    own = rows // 4
    depth = up.shape[0]
    width = down.shape[1]
    cols = up.shape[1]
    wide = n * width
    part = width // 2
    chunk = (depth // 2 // CHUNKS, down.shape[0] // 2 // (CHUNKS // 2))

    barrier = pltpu.get_barrier_semaphore()
    for step in range(1, 4):
        pl.semaphore_signal(
            barrier,
            inc=1,
            device_id={"tp": lax.rem(me + step, 4)},
            device_id_type=pl.DeviceIdType.MESH,
        )
    pl.semaphore_signal(
        barrier, inc=1, device_id={"grp": 1 - y}, device_id_type=pl.DeviceIdType.MESH
    )

    @pl.when(z > 0)
    def _():
        pl.semaphore_signal(
            barrier, inc=1, device_id={"sp": z - 1}, device_id_type=pl.DeviceIdType.MESH
        )

    @pl.when(z < n - 1)
    def _():
        pl.semaphore_signal(
            barrier, inc=1, device_id={"sp": z + 1}, device_id_type=pl.DeviceIdType.MESH
        )

    own_up = up_buf.at[pl.ds(aligned(z, depth), depth), :]
    locals_ = [
        pltpu.make_async_copy(keys, k_buf.at[:, pl.ds(WINDOW, rows)], local_sem.at[0]),
        pltpu.make_async_copy(values, v_buf.at[:, pl.ds(WINDOW, rows)], local_sem.at[1]),
        pltpu.make_async_copy(queries, q_buf, local_sem.at[2]),
        pltpu.make_async_copy(out_weight, ow_buf, local_sem.at[3]),
        pltpu.make_async_copy(residual, res_buf, local_sem.at[4]),
        pltpu.make_async_copy(up, own_up, local_sem.at[5]),
        pltpu.make_async_copy(down.at[:, pl.ds(0, part)], down_buf.at[z, 0], local_sem.at[6]),
        pltpu.make_async_copy(down.at[:, pl.ds(part, part)], down_buf.at[z, 1], local_sem.at[7]),
    ]
    for copy in locals_:
        copy.start()

    edge = jnp.where(z > 0, 1, 0) + jnp.where(z < n - 1, 1, 0)
    pl.semaphore_wait(barrier, 4 + edge)

    def piece(weight, owner, half, index):
        if weight == 0:
            start = owner * depth + half * (depth // 2) + index * chunk[0]
            return up_buf.at[pl.ds(pl.multiple_of(start, chunk[0]), chunk[0]), :]
        start = half * (2 * chunk[1]) + (index % 2) * chunk[1]
        return down_buf.at[
            owner, index // 2, pl.ds(pl.multiple_of(start, chunk[1]), chunk[1]), :
        ]

    def own_piece(weight, index):
        if weight == 0:
            start = y * (CHUNKS * chunk[0]) + index * chunk[0]
            return up.at[pl.ds(pl.multiple_of(start, chunk[0]), chunk[0]), :]
        start = y * (2 * chunk[1]) + (index % 2) * chunk[1]
        return down.at[
            pl.ds(pl.multiple_of(start, chunk[1]), chunk[1]),
            pl.ds(index // 2 * (width // 2), width // 2),
        ]

    def z_copy(weight, owner, index, upward, source=None):
        place = piece(weight, owner, y, index)
        return remote(
            place if source is None else source,
            place,
            z_send.at[upward, weight, owner, index],
            w_recv.at[weight, owner, y, index],
            {"sp": z + (1 if upward else -1)},
        )

    def y_copy(weight, owner, index):
        place = piece(weight, owner, y, index)
        return remote(
            place,
            place,
            y_send.at[weight, owner, index],
            w_recv.at[weight, owner, y, index],
            {"grp": 1 - y},
        )

    def wait_piece(weight, owner, half, index):
        place = piece(weight, owner, half, index)
        remote(
            place,
            place,
            y_send.at[weight, owner, index],
            w_recv.at[weight, owner, half, index],
            {"grp": 1 - y},
        ).wait_recv()

    def send_own(weight, upward):
        for index in range(CHUNKS):
            z_copy(weight, z, index, upward, own_piece(weight, index)).start()

    def tail_copy(which):
        source, place = ((keys, k_buf), (values, v_buf))[which]
        return remote(
            source.at[:, pl.ds(rows - WINDOW, WINDOW)],
            place.at[:, pl.ds(0, WINDOW)],
            tail_send.at[which],
            tail_recv.at[which],
            {"sp": z + 1},
        )

    @pl.when(z < n - 1)
    def _():
        tail_copy(0).start()
        tail_copy(1).start()
        send_own(0, 1)

    @pl.when(z > 0)
    def _():
        send_own(0, 0)

    def send_down(stage):
        @pl.when((z == stage) & (z < n - 1))
        def _():
            send_own(1, 1)

        @pl.when((n - 1 - z == stage) & (z > 0))
        def _():
            send_own(1, 0)

    send_down(0)

    near = jnp.minimum(z, n - 1 - z)
    far_sign = jnp.where(z < n - 1 - z, 1, -1)

    def owner_at(order):
        close = order <= 2 * near
        side = 2 * lax.rem(order + 1, 2) - 1
        return z + jnp.where(close, side * ((order + 1) // 2), far_sign * (order - near))

    def shard_at(number):
        span = 2 * CHUNKS
        close = number < near * span
        rest = number - near * span
        side = 2 * (number % 2) - 1
        owner = z + jnp.where(
            close,
            side * (number // span + 1),
            far_sign * (near + 1 + lax.div(jnp.maximum(rest, 0), CHUNKS)),
        )
        index = jnp.where(
            close, (number % span) // 2, lax.rem(jnp.maximum(rest, 0), CHUNKS)
        )
        return owner, index

    def event(weight, number):
        owner, index = shard_at(number)
        wait_piece(weight, owner, y, index)

        @pl.when((owner < z) & (z < n - 1))
        def _():
            z_copy(weight, owner, index, 1).start()

        @pl.when((owner > z) & (z > 0))
        def _():
            z_copy(weight, owner, index, 0).start()

        y_copy(weight, owner, index).start()

    total_events = (n - 1) * CHUNKS
    done = [0]
    halves = [0]

    def pump(until):
        while done[0] < min(until, 2 * total_events):
            weight, number = divmod(done[0], total_events)
            event(weight, number)
            done[0] += 1
            for stage in range(1, n - 1):
                if done[0] == min(stage * 2 * CHUNKS, total_events):
                    send_down(stage)

    def take_halves(until):
        while halves[0] < until:
            pump(halves[0] + 1 + LEAD)
            weight, number = divmod(halves[0], total_events)
            owner, index = shard_at(number)
            wait_piece(weight, owner, 1 - y, index)
            halves[0] += 1

    @pl.when(z == 0)
    def _():
        k_buf[:, pl.ds(0, WINDOW)] = jnp.zeros((HEAD_DIM, WINDOW), BF16)
        v_buf[:, pl.ds(0, WINDOW)] = jnp.zeros((HEAD_DIM, WINDOW), BF16)

    for copy in locals_[:3]:
        copy.wait()

    @pl.when(z > 0)
    def _():
        tail_copy(0).wait_recv()
        tail_copy(1).wait_recv()

    heads = head_cols // HEAD_DIM
    for h in range(heads):
        k_wide[h * HEAD_DIM : (h + 1) * HEAD_DIM, :] = k_buf[...]
        v_wide[h * HEAD_DIM : (h + 1) * HEAD_DIM, :] = v_buf[...]

    def attend(block, carry):
        start = aligned(block, WINDOW)
        q_rows = q_buf[pl.ds(start, WINDOW), :].astype(F32)
        lane_head = lax.broadcasted_iota(jnp.int32, (WINDOW, head_cols), 1) // HEAD_DIM
        stacked = jnp.concatenate(
            [jnp.where(lane_head == h, q_rows, 0.0) for h in range(heads)], axis=0
        ).astype(BF16)
        scores = jnp.dot(
            stacked, k_wide[:, pl.ds(start, 2 * WINDOW)], preferred_element_type=F32
        ) * HEAD_DIM ** (-0.5)
        i = lax.broadcasted_iota(jnp.int32, (heads * WINDOW, 2 * WINDOW), 0) % WINDOW
        j = lax.broadcasted_iota(jnp.int32, (heads * WINDOW, 2 * WINDOW), 1)
        first = WINDOW - z * rows - block * WINDOW
        valid = (j > i) & (j <= i + WINDOW) & (j >= first)
        scores = jnp.where(valid, scores, -1e30)
        sinks = jnp.concatenate(
            [jnp.full((WINDOW, 1), sink[h], F32) for h in range(heads)], axis=0
        )
        top = jnp.maximum(jnp.max(scores, axis=-1, keepdims=True), sinks)
        weights = jnp.exp(scores - top)
        total = jnp.sum(weights, axis=-1, keepdims=True) + jnp.exp(sinks - top)
        probs = (weights / total).astype(BF16)
        mixed_heads = lax.dot_general(
            probs,
            v_wide[:, pl.ds(start, 2 * WINDOW)],
            (((1,), (1,)), ((), ())),
            preferred_element_type=F32,
        )
        result = jnp.zeros((WINDOW, head_cols), F32)
        for h in range(heads):
            result += jnp.where(
                lane_head == h, mixed_heads[h * WINDOW : (h + 1) * WINDOW], 0.0
            )
        attended[pl.ds(start, WINDOW), :] = result.astype(BF16)
        return carry

    blocks = rows // WINDOW
    for block in range(0, blocks, 2):
        lax.fori_loop(block, min(block + 2, blocks), attend, 0)
        if block + 2 < blocks:
            pump(block // 2 + 1)

    def att_copy(step):
        peer = lax.rem(me + step, 4)
        return remote(
            attended.at[pl.ds(aligned(peer, own), own), :],
            att_all.at[me],
            att_send.at[step - 1],
            att_recv.at[me],
            {"tp": peer},
        )

    def att_wait(step):
        peer = lax.rem(me + step, 4)
        remote(
            att_all.at[peer], att_all.at[peer], att_send.at[step - 1], att_recv.at[peer], {"tp": peer}
        ).wait_recv()

    for step in (2, 1, 3):
        att_copy(step).start()
    att_all[me] = attended[pl.ds(aligned(me, own), own), :]
    pump(4)
    locals_[3].wait()
    locals_[4].wait()
    for step in (1, 2, 3):
        att_wait(step)

    tile = 256

    def project(index, squares):
        span = pl.ds(aligned(index, tile), tile)
        value = res_buf[:, span].astype(F32)
        for peer in range(4):
            value += jnp.dot(
                att_all[peer],
                ow_buf[peer * head_cols : (peer + 1) * head_cols, span],
                preferred_element_type=F32,
            )
        value = value.astype(BF16).astype(F32)
        mixed[:, span] = value
        return squares + jnp.sum(value * value, axis=-1, keepdims=True)

    squares = lax.fori_loop(0, wide // tile, project, jnp.zeros((own, 1), F32))
    scale = lax.rsqrt(squares / wide + 1e-06)
    own_rows = pl.ds(aligned(me, own), own)

    def normalize(index, carry):
        span = pl.ds(aligned(index, tile), tile)
        normed[own_rows, span] = (mixed[:, span] * scale * gain[:, span]).astype(BF16)
        return carry

    lax.fori_loop(0, wide // tile, normalize, 0)

    def norm_copy(slot, source, target):
        place = normed.at[pl.ds(aligned(source, own), own), :]
        return remote(place, place, norm_send.at[slot], norm_recv.at[source], {"tp": target})

    norm_copy(0, me, across).start()
    norm_copy(1, me, partner).start()
    pump(total_events)
    norm_copy(2, across, across).wait_recv()
    norm_copy(2, across, partner).start()

    locals_[5].wait()
    norm_copy(2, partner, partner).wait_recv()
    norm_copy(2, diagonal, partner).wait_recv()

    for order in range(n):
        owner = owner_at(order) if order else z
        if order:
            take_halves(min(order + order % 2, n - 1) * CHUNKS)

        def up_step(index, carry, owner=owner, order=order):
            span = pl.ds(aligned(index, tile), tile)
            value = jnp.dot(
                normed[:, pl.ds(aligned(owner, depth), depth)],
                up_buf[pl.ds(aligned(owner, depth), depth), span],
                preferred_element_type=F32,
            )
            if order:
                value += acc[:, span]
            if order == n - 1:
                hidden[:, span] = jnp.square(jnp.maximum(value, 0.0)).astype(BF16)
            else:
                acc[:, span] = value
            return carry

        lax.fori_loop(0, cols // tile, up_step, 0)

    pieces = [(order, slice(0, width)) for order in range(n - 1)]
    pieces += [(n - 1, slice(0, part)), (n - 1, slice(part, width))]

    def pair_copy(which, slot):
        order, span = pieces[which]
        group = (partner, diagonal)[slot]
        return remote(
            terms.at[order, pl.ds(aligned(group, own), own), span],
            pair_in.at[order, slot, :, span],
            pair_send.at[which, slot],
            pair_recv.at[which, slot],
            {"tp": partner},
        )

    def peer_copy(which):
        order, span = pieces[which]
        return remote(
            chip_sum.at[order, :, span],
            peer_in.at[order, :, span],
            peer_send.at[which],
            peer_recv.at[which],
            {"tp": across},
        )

    def finish(which):
        order, span = pieces[which]
        owner = owner_at(order) if order else z
        size = span.stop - span.start
        target = pl.ds(pl.multiple_of(owner * width + span.start, size), size)
        peer_copy(which).wait_recv()
        pair_copy(which, 0).wait_recv()
        total = (
            terms[order, own_rows, span].astype(F32)
            + pair_in[order, 0, :, span].astype(F32)
            + peer_in[order, :, span].astype(F32)
        )
        out[:, target] = (mixed[:, target] + total).astype(BF16)

    locals_[6].wait()
    locals_[7].wait()
    for which, (order, span) in enumerate(pieces):
        owner = owner_at(order) if order else z
        if order:
            whole = min(order + order % 2, n - 1) * CHUNKS
            last = order == n - 1 and span.stop < width
            take_halves(total_events + whole - (CHUNKS // 2 if last and n % 2 == 0 else 0))
        for index in range(span.start // part, span.stop // part):
            terms[order, :, index * part : (index + 1) * part] = jnp.dot(
                hidden[...], down_buf[owner, index], preferred_element_type=F32
            ).astype(BF16)
        pair_copy(which, 1).start()
        pair_copy(which, 0).start()
        pair_copy(which, 1).wait_recv()
        other = pl.ds(aligned(across, own), own)
        chip_sum[order, :, span] = (
            terms[order, other, span].astype(F32) + pair_in[order, 1, :, span].astype(F32)
        ).astype(BF16)
        peer_copy(which).start()
        if which:
            finish(which - 1)
    finish(len(pieces) - 1)

    for step in (1, 2, 3):
        att_copy(step).wait_send()
    norm_copy(0, me, across).wait_send()
    norm_copy(1, me, partner).wait_send()
    norm_copy(2, across, partner).wait_send()
    for which in range(len(pieces)):
        pair_copy(which, 0).wait_send()
        pair_copy(which, 1).wait_send()
        peer_copy(which).wait_send()

    @pl.when(z < n - 1)
    def _():
        tail_copy(0).wait_send()
        tail_copy(1).wait_send()

    for weight in range(2):
        for owner in range(n):

            @pl.when((z >= owner) & (z < n - 1))
            def _():
                for index in range(CHUNKS):
                    z_copy(weight, owner, index, 1).wait_send()

            @pl.when((z <= owner) & (z > 0))
            def _():
                for index in range(CHUNKS):
                    z_copy(weight, owner, index, 0).wait_send()

            @pl.when(z != owner)
            def _():
                for index in range(CHUNKS):
                    y_copy(weight, owner, index).wait_send()


def fused_body(
    n,
    queries,
    key_rows,
    value_rows,
    sink_logits,
    out_weight,
    residual,
    norm_gain,
    up_weight,
    down_weight,
):
    rows, head_cols = queries.shape
    own, wide = residual.shape
    depth, cols = up_weight.shape
    width = down_weight.shape[1]
    vmem = lambda *shape: pltpu.VMEM(shape, BF16)
    dma = lambda *shape: pltpu.SemaphoreType.DMA(shape)
    hbm = pl.BlockSpec(memory_space=pl.ANY)
    return pl.pallas_call(
        functools.partial(layer_kernel, n),
        out_shape=jax.ShapeDtypeStruct((own, wide), BF16),
        in_specs=[
            hbm,
            hbm,
            hbm,
            pl.BlockSpec(memory_space=pltpu.SMEM),
            hbm,
            hbm,
            pl.BlockSpec(memory_space=pltpu.VMEM),
            hbm,
            hbm,
        ],
        out_specs=pl.BlockSpec(memory_space=pltpu.VMEM),
        scratch_shapes=[
            vmem(rows, head_cols),
            vmem(HEAD_DIM, rows + WINDOW),
            vmem(HEAD_DIM, rows + WINDOW),
            vmem(head_cols, rows + WINDOW),
            vmem(head_cols, rows + WINDOW),
            vmem(rows, head_cols),
            vmem(4, own, head_cols),
            vmem(*out_weight.shape),
            vmem(own, wide),
            pltpu.VMEM((own, wide), F32),
            vmem(rows, wide),
            vmem(n * depth, cols),
            vmem(n, 2, cols, width // 2),
            pltpu.VMEM((rows, cols), F32),
            vmem(rows, cols),
            vmem(n, rows, width),
            vmem(n, 2, own, width),
            vmem(n, own, width),
            vmem(n, own, width),
            dma(8),
            dma(2),
            dma(2),
            dma(2, 2, n, CHUNKS),
            dma(2, n, CHUNKS),
            dma(2, n, 2, CHUNKS),
            dma(3),
            dma(4),
            dma(3),
            dma(4),
            dma(n + 1, 2),
            dma(n + 1, 2),
            dma(n + 1),
            dma(n + 1),
        ],
        compiler_params=pltpu.CompilerParams(
            collective_id=0, has_side_effects=True, vmem_limit_bytes=60 * 1024 * 1024
        ),
    )(
        queries,
        key_rows.T,
        value_rows.T,
        sink_logits,
        out_weight,
        residual,
        norm_gain.reshape(1, -1),
        up_weight,
        down_weight,
    )


def solution(mesh):
    in_specs = (
        P(("grp", "sp"), "tp"),
        P(("grp", "sp"), "tp"),
        P(("grp", "sp"), "tp"),
        P("tp"),
        P(),
        P(("grp", "sp", "tp"), None),
        P(),
        P("sp", "tp"),
        P("tp", "sp"),
    )
    out_specs = P(("grp", "sp", "tp"), None)
    n = mesh.shape["sp"]
    shards_fit = 2 <= n <= 8

    def layer(*arrays):
        key_rows, up_weight, down_weight = arrays[1], arrays[7], arrays[8]
        fits = (
            shards_fit
            and mesh.shape["grp"] == 2
            and mesh.shape["tp"] == 4
            and key_rows.shape[1] == HEAD_DIM
            and up_weight.shape[0] % (32 * CHUNKS) == 0
            and up_weight.shape[1] % 256 == 0
            and down_weight.shape[1] % 256 == 0
        )
        return (functools.partial(fused_body, n) if fits else body)(*arrays)

    return jax.shard_map(layer, mesh=mesh, in_specs=in_specs, out_specs=out_specs, check_vma=False)
```

```python
import functools

import jax
import jax.numpy as jnp
from jax import lax
from jax.experimental import pallas as pl
from jax.experimental.pallas import tpu as pltpu
from jax.sharding import PartitionSpec as P

HEAD_DIM = 64
WINDOW = 128


def shifted(value, axis, steps):
    count = lax.axis_size(axis)
    leading, last = (max(0, -steps), min(count, count - steps))
    return lax.ppermute(value, axis, [(source, source + steps) for source in range(leading, last)])


def band_attend(queries, key_rows, value_rows, sink_logits, tail_keys, tail_values, offset):
    rows = queries.shape[0]
    kv_heads = key_rows.shape[1] // HEAD_DIM
    group = queries.shape[1] // (kv_heads * HEAD_DIM)
    blocks = rows // WINDOW
    all_keys = jnp.concatenate([tail_keys, key_rows], axis=0).reshape(
        blocks + 1, WINDOW, kv_heads, HEAD_DIM
    )
    all_values = jnp.concatenate([tail_values, value_rows], axis=0).reshape(
        blocks + 1, WINDOW, kv_heads, HEAD_DIM
    )
    key_blocks = jnp.concatenate([all_keys[:-1], all_keys[1:]], axis=1)
    value_blocks = jnp.concatenate([all_values[:-1], all_values[1:]], axis=1)
    query_blocks = queries.reshape(blocks, WINDOW, kv_heads, group, HEAD_DIM)
    scores = jnp.einsum(
        "nqkgd,nskd->nkgqs", query_blocks, key_blocks, preferred_element_type=jnp.float32
    ) * HEAD_DIM ** (-0.5)
    q_local = jnp.arange(WINDOW, dtype=jnp.int32) + WINDOW
    k_local = jnp.arange(2 * WINDOW, dtype=jnp.int32)
    distance = q_local[:, None] - k_local[None, :]
    key_position = (
        offset + (jnp.arange(blocks, dtype=jnp.int32)[:, None] - 1) * WINDOW + k_local[None, :]
    )
    valid = ((distance >= 0) & (distance < WINDOW))[None] & (key_position >= 0)[:, None, :]
    scores = jnp.where(valid[:, None, None], scores, -1e30)
    sink = sink_logits.reshape(kv_heads, group)[None, :, :, None, None]
    top = jnp.maximum(jnp.max(scores, axis=-1, keepdims=True), sink)
    weights = jnp.exp(scores - top)
    total = jnp.sum(weights, axis=-1, keepdims=True) + jnp.exp(sink - top)
    probs = (weights / total).astype(jnp.bfloat16)
    result = jnp.einsum(
        "nkgqs,nskd->nqkgd", probs, value_blocks, preferred_element_type=jnp.float32
    )
    return result.astype(jnp.bfloat16).reshape(rows, kv_heads * group * HEAD_DIM)


def body(
    queries,
    key_rows,
    value_rows,
    sink_logits,
    out_weight,
    residual,
    norm_gain,
    up_weight,
    down_weight,
):
    rows = queries.shape[0]
    width = key_rows.shape[1]
    kv_pair = jnp.concatenate([key_rows[rows - WINDOW :], value_rows[rows - WINDOW :]], axis=1)
    tail = shifted(kv_pair, "sp", 1)
    offset = lax.axis_index("sp") * rows
    attended = band_attend(
        queries, key_rows, value_rows, sink_logits, tail[:, :width], tail[:, width:], offset
    )
    head_cols = attended.shape[1]
    own_rows = lax.dynamic_slice_in_dim(out_weight, lax.axis_index("tp") * head_cols, head_cols, 0)
    projected = lax.psum_scatter(
        jnp.dot(attended, own_rows, preferred_element_type=jnp.float32).astype(jnp.bfloat16),
        "tp",
        scatter_dimension=0,
        tiled=True,
    ).astype(jnp.float32)
    mixed32 = (residual.astype(jnp.float32) + projected).astype(jnp.bfloat16).astype(jnp.float32)
    scale = lax.rsqrt(jnp.mean(mixed32 * mixed32, axis=-1, keepdims=True) + 1e-06)
    normed = (mixed32 * scale * norm_gain).astype(jnp.bfloat16)
    all_rows = lax.all_gather(normed, "tp", axis=0, tiled=True)
    before = jnp.dot(
        all_rows,
        lax.all_gather(up_weight, "sp", axis=0, tiled=True),
        preferred_element_type=jnp.float32,
    )
    hidden = jnp.square(jax.nn.relu(before)).astype(jnp.bfloat16)
    terms = jnp.dot(
        hidden,
        lax.all_gather(down_weight, "sp", axis=1, tiled=True),
        preferred_element_type=jnp.float32,
    )
    down = lax.psum_scatter(
        terms.astype(jnp.bfloat16), "tp", scatter_dimension=0, tiled=True
    ).astype(jnp.float32)
    return (mixed32 + down).astype(jnp.bfloat16)


CHUNKS = 4
LEAD = 4
F32 = jnp.float32
BF16 = jnp.bfloat16


def remote(src, dst, send_sem, recv_sem, device_id):
    return pltpu.make_async_remote_copy(
        src_ref=src,
        dst_ref=dst,
        send_sem=send_sem,
        recv_sem=recv_sem,
        device_id=device_id,
        device_id_type=pl.DeviceIdType.MESH,
    )


def aligned(value, size):
    return pl.multiple_of(value * size, size)


def layer_kernel(
    n,
    queries,
    keys,
    values,
    sink,
    out_weight,
    residual,
    gain,
    up,
    down,
    out,
    q_buf,
    k_buf,
    v_buf,
    k_wide,
    v_wide,
    attended,
    att_all,
    ow_buf,
    res_buf,
    mixed,
    normed,
    up_buf,
    down_buf,
    acc,
    hidden,
    terms,
    pair_in,
    chip_sum,
    peer_in,
    local_sem,
    tail_send,
    tail_recv,
    z_send,
    y_send,
    w_recv,
    att_send,
    att_recv,
    norm_send,
    norm_recv,
    pair_send,
    pair_recv,
    peer_send,
    peer_recv,
):
    z = lax.axis_index("sp")
    y = lax.axis_index("grp")
    me = lax.axis_index("tp")
    partner = me + 1 - 2 * lax.rem(me, 2)
    across = lax.rem(me + 2, 4)
    diagonal = lax.rem(partner + 2, 4)
    rows, head_cols = q_buf.shape
    own = rows // 4
    depth = up.shape[0]
    width = down.shape[1]
    cols = up.shape[1]
    wide = n * width
    part = width // 2
    chunk = (depth // 2 // CHUNKS, down.shape[0] // 2 // (CHUNKS // 2))

    barrier = pltpu.get_barrier_semaphore()
    for step in range(1, 4):
        pl.semaphore_signal(
            barrier,
            inc=1,
            device_id={"tp": lax.rem(me + step, 4)},
            device_id_type=pl.DeviceIdType.MESH,
        )
    pl.semaphore_signal(
        barrier, inc=1, device_id={"grp": 1 - y}, device_id_type=pl.DeviceIdType.MESH
    )

    @pl.when(z > 0)
    def _():
        pl.semaphore_signal(
            barrier, inc=1, device_id={"sp": z - 1}, device_id_type=pl.DeviceIdType.MESH
        )

    @pl.when(z < n - 1)
    def _():
        pl.semaphore_signal(
            barrier, inc=1, device_id={"sp": z + 1}, device_id_type=pl.DeviceIdType.MESH
        )

    own_up = up_buf.at[pl.ds(aligned(z, depth), depth), :]
    locals_ = [
        pltpu.make_async_copy(keys, k_buf.at[:, pl.ds(WINDOW, rows)], local_sem.at[0]),
        pltpu.make_async_copy(values, v_buf.at[:, pl.ds(WINDOW, rows)], local_sem.at[1]),
        pltpu.make_async_copy(queries, q_buf, local_sem.at[2]),
        pltpu.make_async_copy(out_weight, ow_buf, local_sem.at[3]),
        pltpu.make_async_copy(residual, res_buf, local_sem.at[4]),
        pltpu.make_async_copy(up, own_up, local_sem.at[5]),
        pltpu.make_async_copy(down.at[:, pl.ds(0, part)], down_buf.at[z, 0], local_sem.at[6]),
        pltpu.make_async_copy(down.at[:, pl.ds(part, part)], down_buf.at[z, 1], local_sem.at[7]),
    ]
    for copy in locals_:
        copy.start()

    edge = jnp.where(z > 0, 1, 0) + jnp.where(z < n - 1, 1, 0)
    pl.semaphore_wait(barrier, 4 + edge)

    def piece(weight, owner, half, index):
        if weight == 0:
            start = owner * depth + half * (depth // 2) + index * chunk[0]
            return up_buf.at[pl.ds(pl.multiple_of(start, chunk[0]), chunk[0]), :]
        start = half * (2 * chunk[1]) + (index % 2) * chunk[1]
        return down_buf.at[
            owner, index // 2, pl.ds(pl.multiple_of(start, chunk[1]), chunk[1]), :
        ]

    def own_piece(weight, index):
        if weight == 0:
            start = y * (CHUNKS * chunk[0]) + index * chunk[0]
            return up.at[pl.ds(pl.multiple_of(start, chunk[0]), chunk[0]), :]
        start = y * (2 * chunk[1]) + (index % 2) * chunk[1]
        return down.at[
            pl.ds(pl.multiple_of(start, chunk[1]), chunk[1]),
            pl.ds(index // 2 * (width // 2), width // 2),
        ]

    def z_copy(weight, owner, index, upward, source=None):
        place = piece(weight, owner, y, index)
        return remote(
            place if source is None else source,
            place,
            z_send.at[upward, weight, owner, index],
            w_recv.at[weight, owner, y, index],
            {"sp": z + (1 if upward else -1)},
        )

    def y_copy(weight, owner, index):
        place = piece(weight, owner, y, index)
        return remote(
            place,
            place,
            y_send.at[weight, owner, index],
            w_recv.at[weight, owner, y, index],
            {"grp": 1 - y},
        )

    def wait_piece(weight, owner, half, index):
        place = piece(weight, owner, half, index)
        remote(
            place,
            place,
            y_send.at[weight, owner, index],
            w_recv.at[weight, owner, half, index],
            {"grp": 1 - y},
        ).wait_recv()

    def send_own(weight, upward):
        for index in range(CHUNKS):
            z_copy(weight, z, index, upward, own_piece(weight, index)).start()

    def tail_copy(which):
        source, place = ((keys, k_buf), (values, v_buf))[which]
        return remote(
            source.at[:, pl.ds(rows - WINDOW, WINDOW)],
            place.at[:, pl.ds(0, WINDOW)],
            tail_send.at[which],
            tail_recv.at[which],
            {"sp": z + 1},
        )

    @pl.when(z < n - 1)
    def _():
        tail_copy(0).start()
        tail_copy(1).start()
        send_own(0, 1)

    @pl.when(z > 0)
    def _():
        send_own(0, 0)

    def send_down(stage):
        @pl.when((z == stage) & (z < n - 1))
        def _():
            send_own(1, 1)

        @pl.when((n - 1 - z == stage) & (z > 0))
        def _():
            send_own(1, 0)

    send_down(0)

    near = jnp.minimum(z, n - 1 - z)
    far_sign = jnp.where(z < n - 1 - z, 1, -1)

    def owner_at(order):
        close = order <= 2 * near
        side = 2 * lax.rem(order + 1, 2) - 1
        return z + jnp.where(close, side * ((order + 1) // 2), far_sign * (order - near))

    def shard_at(number):
        span = 2 * CHUNKS
        close = number < near * span
        rest = number - near * span
        side = 2 * (number % 2) - 1
        owner = z + jnp.where(
            close,
            side * (number // span + 1),
            far_sign * (near + 1 + lax.div(jnp.maximum(rest, 0), CHUNKS)),
        )
        index = jnp.where(
            close, (number % span) // 2, lax.rem(jnp.maximum(rest, 0), CHUNKS)
        )
        return owner, index

    def event(weight, number):
        owner, index = shard_at(number)
        wait_piece(weight, owner, y, index)

        @pl.when((owner < z) & (z < n - 1))
        def _():
            z_copy(weight, owner, index, 1).start()

        @pl.when((owner > z) & (z > 0))
        def _():
            z_copy(weight, owner, index, 0).start()

        y_copy(weight, owner, index).start()

    total_events = (n - 1) * CHUNKS
    done = [0]
    halves = [0]

    def pump(until):
        while done[0] < min(until, 2 * total_events):
            weight, number = divmod(done[0], total_events)
            event(weight, number)
            done[0] += 1
            for stage in range(1, n - 1):
                if done[0] == min(stage * 2 * CHUNKS, total_events):
                    send_down(stage)

    def take_halves(until):
        while halves[0] < until:
            pump(halves[0] + 1 + LEAD)
            weight, number = divmod(halves[0], total_events)
            owner, index = shard_at(number)
            wait_piece(weight, owner, 1 - y, index)
            halves[0] += 1

    @pl.when(z == 0)
    def _():
        k_buf[:, pl.ds(0, WINDOW)] = jnp.zeros((HEAD_DIM, WINDOW), BF16)
        v_buf[:, pl.ds(0, WINDOW)] = jnp.zeros((HEAD_DIM, WINDOW), BF16)

    for copy in locals_[:3]:
        copy.wait()

    @pl.when(z > 0)
    def _():
        tail_copy(0).wait_recv()
        tail_copy(1).wait_recv()

    heads = head_cols // HEAD_DIM
    for h in range(heads):
        k_wide[h * HEAD_DIM : (h + 1) * HEAD_DIM, :] = k_buf[...]
        v_wide[h * HEAD_DIM : (h + 1) * HEAD_DIM, :] = v_buf[...]

    def attend(block, carry):
        start = aligned(block, WINDOW)
        q_rows = q_buf[pl.ds(start, WINDOW), :].astype(F32)
        lane_head = lax.broadcasted_iota(jnp.int32, (WINDOW, head_cols), 1) // HEAD_DIM
        stacked = jnp.concatenate(
            [jnp.where(lane_head == h, q_rows, 0.0) for h in range(heads)], axis=0
        ).astype(BF16)
        scores = jnp.dot(
            stacked, k_wide[:, pl.ds(start, 2 * WINDOW)], preferred_element_type=F32
        ) * HEAD_DIM ** (-0.5)
        i = lax.broadcasted_iota(jnp.int32, (heads * WINDOW, 2 * WINDOW), 0) % WINDOW
        j = lax.broadcasted_iota(jnp.int32, (heads * WINDOW, 2 * WINDOW), 1)
        first = WINDOW - z * rows - block * WINDOW
        valid = (j > i) & (j <= i + WINDOW) & (j >= first)
        scores = jnp.where(valid, scores, -1e30)
        sinks = jnp.concatenate(
            [jnp.full((WINDOW, 1), sink[h], F32) for h in range(heads)], axis=0
        )
        top = jnp.maximum(jnp.max(scores, axis=-1, keepdims=True), sinks)
        weights = jnp.exp(scores - top)
        total = jnp.sum(weights, axis=-1, keepdims=True) + jnp.exp(sinks - top)
        probs = (weights / total).astype(BF16)
        mixed_heads = lax.dot_general(
            probs,
            v_wide[:, pl.ds(start, 2 * WINDOW)],
            (((1,), (1,)), ((), ())),
            preferred_element_type=F32,
        )
        result = jnp.zeros((WINDOW, head_cols), F32)
        for h in range(heads):
            result += jnp.where(
                lane_head == h, mixed_heads[h * WINDOW : (h + 1) * WINDOW], 0.0
            )
        attended[pl.ds(start, WINDOW), :] = result.astype(BF16)
        return carry

    blocks = rows // WINDOW
    for block in range(0, blocks, 2):
        lax.fori_loop(block, min(block + 2, blocks), attend, 0)
        if block + 2 < blocks:
            pump(block // 2 + 1)

    def att_copy(step):
        peer = lax.rem(me + step, 4)
        return remote(
            attended.at[pl.ds(aligned(peer, own), own), :],
            att_all.at[me],
            att_send.at[step - 1],
            att_recv.at[me],
            {"tp": peer},
        )

    def att_wait(step):
        peer = lax.rem(me + step, 4)
        remote(
            att_all.at[peer], att_all.at[peer], att_send.at[step - 1], att_recv.at[peer], {"tp": peer}
        ).wait_recv()

    for step in (2, 1, 3):
        att_copy(step).start()
    att_all[me] = attended[pl.ds(aligned(me, own), own), :]
    pump(4)
    locals_[3].wait()
    locals_[4].wait()
    for step in (1, 2, 3):
        att_wait(step)

    tile = 256

    def project(index, squares):
        span = pl.ds(aligned(index, tile), tile)
        value = res_buf[:, span].astype(F32)
        for peer in range(4):
            value += jnp.dot(
                att_all[peer],
                ow_buf[peer * head_cols : (peer + 1) * head_cols, span],
                preferred_element_type=F32,
            )
        value = value.astype(BF16).astype(F32)
        mixed[:, span] = value
        return squares + jnp.sum(value * value, axis=-1, keepdims=True)

    squares = lax.fori_loop(0, wide // tile, project, jnp.zeros((own, 1), F32))
    scale = lax.rsqrt(squares / wide + 1e-06)
    own_rows = pl.ds(aligned(me, own), own)

    def normalize(index, carry):
        span = pl.ds(aligned(index, tile), tile)
        normed[own_rows, span] = (mixed[:, span] * scale * gain[:, span]).astype(BF16)
        return carry

    lax.fori_loop(0, wide // tile, normalize, 0)

    def norm_copy(slot, source, target):
        place = normed.at[pl.ds(aligned(source, own), own), :]
        return remote(place, place, norm_send.at[slot], norm_recv.at[source], {"tp": target})

    norm_copy(0, me, across).start()
    norm_copy(1, me, partner).start()
    pump(total_events + 2)
    norm_copy(2, across, across).wait_recv()
    norm_copy(2, across, partner).start()

    locals_[5].wait()
    norm_copy(2, partner, partner).wait_recv()
    norm_copy(2, diagonal, partner).wait_recv()

    for order in range(n):
        owner = owner_at(order) if order else z
        if order:
            take_halves(min(order + order % 2, n - 1) * CHUNKS)

        def up_step(index, carry, owner=owner, order=order):
            span = pl.ds(aligned(index, tile), tile)
            value = jnp.dot(
                normed[:, pl.ds(aligned(owner, depth), depth)],
                up_buf[pl.ds(aligned(owner, depth), depth), span],
                preferred_element_type=F32,
            )
            if order:
                value += acc[:, span]
            if order == n - 1:
                hidden[:, span] = jnp.square(jnp.maximum(value, 0.0)).astype(BF16)
            else:
                acc[:, span] = value
            return carry

        lax.fori_loop(0, cols // tile, up_step, 0)

    pieces = [(order, slice(0, width)) for order in range(n - 1)]
    pieces += [(n - 1, slice(0, part)), (n - 1, slice(part, width))]

    def pair_copy(which, slot):
        order, span = pieces[which]
        group = (partner, diagonal)[slot]
        return remote(
            terms.at[order, pl.ds(aligned(group, own), own), span],
            pair_in.at[order, slot, :, span],
            pair_send.at[which, slot],
            pair_recv.at[which, slot],
            {"tp": partner},
        )

    def peer_copy(which):
        order, span = pieces[which]
        return remote(
            chip_sum.at[order, :, span],
            peer_in.at[order, :, span],
            peer_send.at[which],
            peer_recv.at[which],
            {"tp": across},
        )

    def finish(which):
        order, span = pieces[which]
        owner = owner_at(order) if order else z
        size = span.stop - span.start
        target = pl.ds(pl.multiple_of(owner * width + span.start, size), size)
        peer_copy(which).wait_recv()
        pair_copy(which, 0).wait_recv()
        total = (
            terms[order, own_rows, span].astype(F32)
            + pair_in[order, 0, :, span].astype(F32)
            + peer_in[order, :, span].astype(F32)
        )
        out[:, target] = (mixed[:, target] + total).astype(BF16)

    locals_[6].wait()
    locals_[7].wait()
    for which, (order, span) in enumerate(pieces):
        owner = owner_at(order) if order else z
        if order:
            whole = min(order + order % 2, n - 1) * CHUNKS
            last = order == n - 1 and span.stop < width
            take_halves(total_events + whole - (CHUNKS // 2 if last and n % 2 == 0 else 0))
        for index in range(span.start // part, span.stop // part):
            terms[order, :, index * part : (index + 1) * part] = jnp.dot(
                hidden[...], down_buf[owner, index], preferred_element_type=F32
            ).astype(BF16)
        pair_copy(which, 1).start()
        pair_copy(which, 0).start()
        pair_copy(which, 1).wait_recv()
        other = pl.ds(aligned(across, own), own)
        chip_sum[order, :, span] = (
            terms[order, other, span].astype(F32) + pair_in[order, 1, :, span].astype(F32)
        ).astype(BF16)
        peer_copy(which).start()
        if which:
            finish(which - 1)
    finish(len(pieces) - 1)

    for step in (1, 2, 3):
        att_copy(step).wait_send()
    norm_copy(0, me, across).wait_send()
    norm_copy(1, me, partner).wait_send()
    norm_copy(2, across, partner).wait_send()
    for which in range(len(pieces)):
        pair_copy(which, 0).wait_send()
        pair_copy(which, 1).wait_send()
        peer_copy(which).wait_send()

    @pl.when(z < n - 1)
    def _():
        tail_copy(0).wait_send()
        tail_copy(1).wait_send()

    for weight in range(2):
        for owner in range(n):

            @pl.when((z >= owner) & (z < n - 1))
            def _():
                for index in range(CHUNKS):
                    z_copy(weight, owner, index, 1).wait_send()

            @pl.when((z <= owner) & (z > 0))
            def _():
                for index in range(CHUNKS):
                    z_copy(weight, owner, index, 0).wait_send()

            @pl.when(z != owner)
            def _():
                for index in range(CHUNKS):
                    y_copy(weight, owner, index).wait_send()


def fused_body(
    n,
    queries,
    key_rows,
    value_rows,
    sink_logits,
    out_weight,
    residual,
    norm_gain,
    up_weight,
    down_weight,
):
    rows, head_cols = queries.shape
    own, wide = residual.shape
    depth, cols = up_weight.shape
    width = down_weight.shape[1]
    vmem = lambda *shape: pltpu.VMEM(shape, BF16)
    dma = lambda *shape: pltpu.SemaphoreType.DMA(shape)
    hbm = pl.BlockSpec(memory_space=pl.ANY)
    return pl.pallas_call(
        functools.partial(layer_kernel, n),
        out_shape=jax.ShapeDtypeStruct((own, wide), BF16),
        in_specs=[
            hbm,
            hbm,
            hbm,
            pl.BlockSpec(memory_space=pltpu.SMEM),
            hbm,
            hbm,
            pl.BlockSpec(memory_space=pltpu.VMEM),
            hbm,
            hbm,
        ],
        out_specs=pl.BlockSpec(memory_space=pltpu.VMEM),
        scratch_shapes=[
            vmem(rows, head_cols),
            vmem(HEAD_DIM, rows + WINDOW),
            vmem(HEAD_DIM, rows + WINDOW),
            vmem(head_cols, rows + WINDOW),
            vmem(head_cols, rows + WINDOW),
            vmem(rows, head_cols),
            vmem(4, own, head_cols),
            vmem(*out_weight.shape),
            vmem(own, wide),
            pltpu.VMEM((own, wide), F32),
            vmem(rows, wide),
            vmem(n * depth, cols),
            vmem(n, 2, cols, width // 2),
            pltpu.VMEM((rows, cols), F32),
            vmem(rows, cols),
            vmem(n, rows, width),
            vmem(n, 2, own, width),
            vmem(n, own, width),
            vmem(n, own, width),
            dma(8),
            dma(2),
            dma(2),
            dma(2, 2, n, CHUNKS),
            dma(2, n, CHUNKS),
            dma(2, n, 2, CHUNKS),
            dma(3),
            dma(4),
            dma(3),
            dma(4),
            dma(n + 1, 2),
            dma(n + 1, 2),
            dma(n + 1),
            dma(n + 1),
        ],
        compiler_params=pltpu.CompilerParams(
            collective_id=0, has_side_effects=True, vmem_limit_bytes=60 * 1024 * 1024
        ),
    )(
        queries,
        key_rows.T,
        value_rows.T,
        sink_logits,
        out_weight,
        residual,
        norm_gain.reshape(1, -1),
        up_weight,
        down_weight,
    )


def solution(mesh):
    in_specs = (
        P(("grp", "sp"), "tp"),
        P(("grp", "sp"), "tp"),
        P(("grp", "sp"), "tp"),
        P("tp"),
        P(),
        P(("grp", "sp", "tp"), None),
        P(),
        P("sp", "tp"),
        P("tp", "sp"),
    )
    out_specs = P(("grp", "sp", "tp"), None)
    n = mesh.shape["sp"]
    shards_fit = 2 <= n <= 8

    def layer(*arrays):
        key_rows, up_weight, down_weight = arrays[1], arrays[7], arrays[8]
        fits = (
            shards_fit
            and mesh.shape["grp"] == 2
            and mesh.shape["tp"] == 4
            and key_rows.shape[1] == HEAD_DIM
            and up_weight.shape[0] % (32 * CHUNKS) == 0
            and up_weight.shape[1] % 256 == 0
            and down_weight.shape[1] % 256 == 0
        )
        return (functools.partial(fused_body, n) if fits else body)(*arrays)

    return jax.shard_map(layer, mesh=mesh, in_specs=in_specs, out_specs=out_specs, check_vma=False)
```
